32 devices in a mesh: rep: 2 (over x), fs: 4 (over z), tp: 4 (over y, core).
Axes of the slice: x: 2, y: 2, z: 4, core: 2. Of those that a mesh axis runs over, the one named last changes fastest.
Arguments:
- tokens: bfloat16 [4096, 2048], P(('rep', 'fs', 'tp')), may hold values from -6 to 6
- norm1_gain: float32 [2048], replicated, may hold values from 0.1 to 1.9
- in_weight: bfloat16 [2048, 1024], P('fs', 'tp'), may hold values from -0.125 to 0.125
- group_weight: bfloat16 [8, 128, 128], P('tp'), may hold values from -0.5 to 0.5
- pool_scale: float32 [1024], P('tp'), may hold values from 0.1 to 1.9
- out_weight: bfloat16 [1024, 2048], P('tp', 'fs'), may hold values from -0.1875 to 0.1875
- norm2_gain: float32 [2048], replicated, may hold values from 0.1 to 1.9
- up_weight: bfloat16 [2048, 8192], P('fs', 'tp'), may hold values from -0.125 to 0.125
- down_weight: bfloat16 [8192, 2048], P('tp', 'fs'), may hold values from -0.0625 to 0.0625
Outputs:
- layer_out: bfloat16 [4096, 2048], P(('rep', 'fs', 'tp'))
The draws below stay inside these ranges and needn't reach their ends.
All inputs are finite; a program needn't handle non-finite values.
Results may differ from the reference program's by a relative error of at most 0.02.
Values may be sent and summed in bfloat16 or wider, within the bound.
A program may use at most 128 MiB of HBM per device.

```python
import jax
import jax.numpy as jnp
from jax import lax

D = 2048
GROUPS = 8
GROUP_DIM = 128
FF = 8192
POOL = 1024
SEQ = 512
TOKENS = 4096
N_TP = 4


def block_levels(own_key, dims, shards, smallest, largest):
    def one(dim, blocks):
        steps = jax.random.uniform(jax.random.fold_in(jax.random.fold_in(own_key, 6), dim), (blocks,), jnp.float32, smallest / len(shards), largest / len(shards))
        return jnp.repeat(jnp.exp(steps), dims[dim] // blocks).reshape((-1,) + (1,) * (len(dims) - dim - 1))

    loudness = one(*shards[0])
    for cut in shards[1:]:
        loudness = loudness * one(*cut)
    return loudness


def normal_values(rng, shape, scale, most, cuts=(), kind=jnp.bfloat16):
    values = scale * jax.random.normal(rng, shape, jnp.float32)
    if cuts:
        values = values * block_levels(rng, shape, cuts, -0.22, 0.18)
    return jnp.clip(values, -most, most).astype(kind)


def setup_inputs(seed: int = 0) -> dict:
    streams_of = jax.random.split(jax.random.key(seed), 10)
    return {
        "tokens": normal_values(streams_of[0], (TOKENS, D), 1.0, 6.0, ((0, 32),)),
        "norm1_gain": jnp.clip(1.0 + 0.18 * jax.random.normal(streams_of[1], (D,), jnp.float32), 0.1, 1.9),
        "in_weight": normal_values(streams_of[2], (D, POOL), D ** -0.5, 0.125, ((0, 4), (1, 4))),
        "group_weight": normal_values(streams_of[3], (GROUPS, GROUP_DIM, GROUP_DIM), GROUP_DIM ** -0.5, 0.5, ((0, 4),)),
        "pool_scale": jnp.clip(1.0 + 0.18 * jax.random.normal(streams_of[4], (POOL,), jnp.float32), 0.1, 1.9),
        "out_weight": normal_values(streams_of[5], (POOL, D), POOL ** -0.5, 0.1875, ((0, 4), (1, 4))),
        "norm2_gain": jnp.clip(1.0 + 0.18 * jax.random.normal(streams_of[6], (D,), jnp.float32), 0.1, 1.9),
        "up_weight": normal_values(streams_of[7], (D, FF), D ** -0.5, 0.125, ((0, 4), (1, 4))),
        "down_weight": normal_values(streams_of[8], (FF, D), FF ** -0.5, 0.0625, ((0, 4), (1, 4))),
    }


epsilon = 1e-06

def rms_norm(values, gain):
    scale = lax.rsqrt(lax.optimization_barrier(jnp.mean(values * values, axis=-1, keepdims=True)) + epsilon)
    return values * scale * gain

def one_sequence(rows, norm1_gain, in_weight, group_weight, pool_scale, out_weight, norm2_gain, up_weight, down_weight):
    stream = rows.astype(jnp.float32)
    normed = rms_norm(stream, norm1_gain).astype(jnp.bfloat16)
    projected = jnp.dot(normed, in_weight, preferred_element_type=jnp.float32).astype(jnp.bfloat16)
    values = projected.astype(jnp.float32).reshape(SEQ, GROUPS, GROUP_DIM)
    totals = jnp.cumsum(values, axis=0)
    padded = jnp.pad(totals, ((16, 0), (0, 0), (0, 0)))
    position = jnp.arange(SEQ, dtype=jnp.int32)[:, None, None]
    group_level = (jnp.arange(GROUPS, dtype=jnp.int32) % 4)[None, :, None]
    window_mean = jnp.zeros((SEQ, GROUPS, GROUP_DIM), jnp.float32)
    for level in range(4):
        width = 2 ** (level + 1)
        sums = totals - padded[16 - width:16 - width + SEQ]
        count = jnp.minimum(position + 1, width).astype(jnp.float32)
        window_mean = jnp.where(group_level == level, sums / count, window_mean)
    pooled = (window_mean - values).astype(jnp.bfloat16)
    mapped = jnp.einsum('sgc,gcd->sgd', pooled.astype(jnp.float32), group_weight.astype(jnp.float32))
    pool_out = (mapped.reshape(SEQ, POOL) * pool_scale).astype(jnp.bfloat16)
    mixed_stream = stream + jnp.dot(pool_out, out_weight, preferred_element_type=jnp.float32)
    normed_two = rms_norm(mixed_stream, norm2_gain).astype(jnp.bfloat16)
    upper = jnp.dot(normed_two, up_weight, preferred_element_type=jnp.float32)
    hidden = jnp.square(jax.nn.relu(upper)).astype(jnp.bfloat16)
    block = FF // N_TP
    channel_sum = jnp.zeros((SEQ, D), jnp.float32)
    for index in range(N_TP):
        partial_sum = jnp.dot(hidden[:, index * block:(index + 1) * block], down_weight[index * block:(index + 1) * block], preferred_element_type=jnp.float32).astype(jnp.bfloat16)
        channel_sum = channel_sum + lax.optimization_barrier(partial_sum).astype(jnp.float32)
    return (mixed_stream + channel_sum).astype(jnp.bfloat16)

def reference(tokens, norm1_gain, in_weight, group_weight, pool_scale, out_weight, norm2_gain, up_weight, down_weight):
    sequences = tokens.reshape(TOKENS // SEQ, SEQ, D)

    def apply(rows):
        return one_sequence(rows, norm1_gain, in_weight, group_weight, pool_scale, out_weight, norm2_gain, up_weight, down_weight)
    return lax.map(apply, sequences).reshape(TOKENS, D)
```

```python
import functools

import jax
import jax.numpy as jnp
from jax import lax
from jax.experimental import pallas as pl
from jax.experimental.pallas import tpu as pltpu
from jax.sharding import PartitionSpec as P

MESH = pl.DeviceIdType.MESH
CHUNK_BYTES = 256 * 1024
LEVELS = 4

epsilon = 1e-06


def chunks_of(rows, columns, parts):
    count = max(1, rows * columns * 2 // parts // CHUNK_BYTES)
    while (rows // parts) % (count * 16):
        count -= 1
    return count


def dot(a, b):
    return jnp.dot(a, b, preferred_element_type=jnp.float32)


def tile_of(columns, most):
    tile = min(columns, most)
    while columns % tile:
        tile //= 2
    return tile


def kernel(
    sizes,
    tokens,
    gain1,
    in_hbm,
    group_weight,
    pool_scale,
    out_hbm,
    gain2,
    up_hbm,
    down_hbm,
    result,
    in_buf,
    out_buf,
    up_buf,
    down_buf,
    normed,
    projected,
    pool_out,
    mix_send,
    mix_recv,
    stream2,
    normed2,
    upper,
    hidden,
    sum_send,
    sum_recv,
    local_sem,
    in_sems,
    out_sems,
    up_sems,
    down_sems,
    tp_send,
    tp_recv,
):
    n_rep, n_fs, n_tp = sizes
    r, f, t = lax.axis_index("rep"), lax.axis_index("fs"), lax.axis_index("tp")
    rows = tokens.shape[0]
    length = rows * n_tp
    width = tokens.shape[1]
    part = width // n_fs
    buffers = (in_buf, out_buf, up_buf, down_buf)
    sources = (in_hbm, out_hbm, up_hbm, down_hbm)
    sems = (
        in_sems,
        out_sems,
        up_sems,
        down_sems,
    )
    chunk_counts = [chunks_of(b.shape[1], b.shape[2], n_rep) for b in buffers]

    loads = []
    for index in range(4):
        load = pltpu.make_async_copy(sources[index], buffers[index].at[f], local_sem.at[index])
        load.start()
        loads.append(load)

    barrier = pltpu.get_barrier_semaphore()
    greeted = [{"fs": lax.rem(f + d, n_fs)} for d in (1, n_fs - 1)]
    greeted += [{"rep": lax.rem(r + d, n_rep)} for d in range(1, n_rep)]
    greeted += [{"tp": lax.rem(t + d, n_tp)} for d in range(1, n_tp)]
    for device in greeted:
        pl.semaphore_signal(barrier, inc=1, device_id=device, device_id_type=MESH)

    def order(p):
        nearest = jnp.minimum(f, n_fs - 1 - f)
        step = (p + 1) // 2
        near = f + step if p % 2 else f - step
        far = f + (p - nearest) * jnp.where(2 * f < n_fs, 1, -1)
        return jnp.where(p <= 2 * nearest, near, far)

    def piece(g, j, q, c):
        buf = buffers[g]
        size = buf.shape[1] // n_rep // chunk_counts[g]
        start = pl.multiple_of((q * chunk_counts[g] + c) * size, size)
        return buf.at[j, pl.ds(start, size), :]

    def remote(g, j, q, c, send_slot, device):
        block = piece(g, j, q, c)
        return pltpu.make_async_remote_copy(
            src_ref=block,
            dst_ref=block,
            send_sem=sems[g].at[j, send_slot, c],
            recv_sem=sems[g].at[j, q, c],
            device_id=device,
            device_id_type=MESH,
        )

    def along(g, j, c, way, act):
        if way == 0:

            @pl.when(f > 0)
            def _():
                act(remote(g, j, r, c, 2 * n_rep, {"fs": f - 1}))

        else:

            @pl.when(f < n_fs - 1)
            def _():
                act(remote(g, j, r, c, 2 * n_rep + 1, {"fs": f + 1}))

    def start(copy):
        copy.start()

    def drain(copy):
        copy.wait_send()

    def onward(g, p, c, act):
        j = order(p)

        @pl.when(j > f)
        def _():
            along(g, j, c, 0, act)

        @pl.when(j < f)
        def _():
            along(g, j, c, 1, act)

        for d in range(1, n_rep):
            other = lax.rem(r + d, n_rep)
            act(remote(g, j, r, c, n_rep + other, {"rep": other}))

    def send_own(g):
        for c in range(chunk_counts[g]):
            along(g, f, c, 0, start)
            along(g, f, c, 1, start)

    def relay(g, p):
        for c in range(chunk_counts[g]):
            j = order(p)
            remote(g, j, r, c, 2 * n_rep, {"fs": f}).wait_recv()
            onward(g, p, c, start)

    def arrived(g, p):
        j = order(p)
        for d in range(1, n_rep):
            other = lax.rem(r + d, n_rep)
            for c in range(chunk_counts[g]):
                remote(g, j, other, c, n_rep + other, {"rep": other}).wait_recv()

    def block_of(index):
        return pl.ds(pl.multiple_of(index * rows, rows), rows)

    def tp_copies(kind, source, target):
        made = []
        for d in range(1, n_tp):
            other = lax.rem(t + d, n_tp)
            made.append(
                pltpu.make_async_remote_copy(
                    src_ref=source(other),
                    dst_ref=target(t),
                    send_sem=tp_send.at[kind, other],
                    recv_sem=tp_recv.at[kind, t],
                    device_id={"tp": other},
                    device_id_type=MESH,
                )
            )
        return made

    def tp_wait(kind, target):
        for d in range(1, n_tp):
            other = lax.rem(t + d, n_tp)
            pltpu.make_async_remote_copy(
                src_ref=target(other),
                dst_ref=target(other),
                send_sem=tp_send.at[kind, other],
                recv_sem=tp_recv.at[kind, other],
                device_id={"tp": other},
                device_id_type=MESH,
            ).wait_recv()

    stream = tokens[...].astype(jnp.float32)
    scale = lax.rsqrt(jnp.mean(stream * stream, axis=-1, keepdims=True) + epsilon)
    normed[block_of(t), :] = (stream * scale * gain1[...]).astype(jnp.bfloat16)

    pl.semaphore_wait(barrier, len(greeted))
    loads[0].wait()
    send_own(0)
    loads[1].wait()
    send_own(1)
    normed_at = lambda index: normed.at[block_of(index), :]
    sends = tp_copies(0, lambda other: normed_at(t), normed_at)
    for copy in sends:
        copy.start()
    for p in range(1, n_fs):
        relay(0, p)
        relay(1, p)
    loads[2].wait()
    send_own(2)

    tp_wait(0, normed_at)
    for p in range(1, n_fs):
        arrived(0, p)
    total = dot(normed[:, :part], in_buf[0])
    for index in range(1, n_fs):
        total += dot(normed[:, index * part : (index + 1) * part], in_buf[index])
    projected[...] = total.astype(jnp.bfloat16).astype(jnp.float32)
    groups, channels = group_weight.shape[0], group_weight.shape[1]
    position = lax.broadcasted_iota(jnp.int32, (length, channels), 0)
    for group in range(groups):
        lanes = slice(group * channels, (group + 1) * channels)
        values = projected[:, lanes]
        level_of = jnp.full((length, channels), lax.rem(t * groups + group, LEVELS), jnp.int32)
        running = values
        mean = jnp.zeros_like(values)
        for level in range(LEVELS):
            offset = 2**level
            running = running + jnp.where(position >= offset, pltpu.roll(running, offset, 0), 0.0)
            count = jnp.minimum(position + 1, 2 * offset).astype(jnp.float32)
            mean = jnp.where(level_of == level, running / count, mean)
        pooled = (mean - values).astype(jnp.bfloat16)
        mapped = dot(pooled, group_weight[group])
        pool_out[:, lanes] = (mapped * pool_scale[:, lanes]).astype(jnp.bfloat16)

    for p in range(1, n_fs):
        arrived(1, p)
    for index in range(n_fs):
        mix_send[index] = dot(pool_out[...], out_buf[index]).astype(jnp.bfloat16)
    more = tp_copies(
        1, lambda other: mix_send.at[:, block_of(other), :], lambda index: mix_recv.at[index]
    )
    relay(2, 1)
    for copy in more:
        copy.start()
    sends += more
    for p in range(2, n_fs - 1):
        relay(2, p)

    tp_wait(1, lambda index: mix_recv.at[index])
    square = jnp.zeros((rows, 1), jnp.float32)
    for index in range(n_fs):
        mixed = tokens[:, index * part : (index + 1) * part].astype(jnp.float32)
        mixed += mix_send[index, block_of(t), :].astype(jnp.float32)
        for d in range(1, n_tp):
            mixed += mix_recv[lax.rem(t + d, n_tp), index].astype(jnp.float32)
        stream2[index] = mixed
        square += jnp.sum(mixed * mixed, axis=-1, keepdims=True)
    scale = lax.rsqrt(square / width + epsilon)
    for index in range(n_fs):
        columns = slice(index * part, (index + 1) * part)
        normed2[block_of(t), columns] = (stream2[index] * scale * gain2[:, columns]).astype(
            jnp.bfloat16
        )
    normed2_at = lambda index: normed2.at[block_of(index), :]
    more = tp_copies(2, lambda other: normed2_at(t), normed2_at)
    for copy in more:
        copy.start()
    sends += more
    if n_fs > 2:
        relay(2, n_fs - 1)
    loads[3].wait()
    send_own(3)

    tp_wait(2, normed2_at)
    up_columns = up_buf.shape[2]
    up_tile = tile_of(up_columns, 512)

    def up_product(p):
        j = order(p)
        left = normed2.at[:, pl.ds(pl.multiple_of(j * part, part), part)]

        @pl.loop(0, up_columns // up_tile)
        def _(i):
            columns = pl.ds(pl.multiple_of(i * up_tile, up_tile), up_tile)
            product = dot(left[...], up_buf[j, :, columns])
            if p == 0:
                upper[:, columns] = product
            elif p < n_fs - 1:
                upper[:, columns] += product
            else:
                value = jnp.maximum(upper[:, columns] + product, 0.0)
                hidden[:, columns] = (value * value).astype(jnp.bfloat16)

    up_product(0)
    for p in range(1, n_fs):
        if p == n_fs - 1:
            relay(3, 1)
        arrived(2, p)
        up_product(p)

    down_tile = tile_of(part, 256)

    def sum_kind(p):
        return 3 + p

    def down_product(p):
        j = order(p)

        @pl.loop(0, part // down_tile)
        def _(i):
            columns = pl.ds(pl.multiple_of(i * down_tile, down_tile), down_tile)
            sum_send[p, :, columns] = dot(hidden[...], down_buf[j, :, columns]).astype(jnp.bfloat16)

        copies = tp_copies(
            sum_kind(p),
            lambda other: sum_send.at[p, block_of(other), :],
            lambda index: sum_recv.at[p, index],
        )
        for copy in copies:
            copy.start()
        return copies

    def finish(p):
        j = order(p)
        tp_wait(sum_kind(p), lambda index: sum_recv.at[p, index])
        channel = sum_send[p, block_of(t), :].astype(jnp.float32)
        for d in range(1, n_tp):
            channel += sum_recv[p, lax.rem(t + d, n_tp)].astype(jnp.float32)
        columns = pl.ds(pl.multiple_of(j * part, part), part)
        result[:, columns] = (stream2[j] + channel).astype(jnp.bfloat16)

    sends += down_product(0)
    for p in range(1, n_fs):
        if p < n_fs - 1:
            relay(3, p + 1)
        arrived(3, p)
        sends += down_product(p)
        finish(p - 1)
    for g in range(4):
        for c in range(chunk_counts[g]):
            along(g, f, c, 0, drain)
            along(g, f, c, 1, drain)
            for p in range(1, n_fs):
                onward(g, p, c, drain)
    finish(n_fs - 1)
    for copy in sends:
        copy.wait_send()


def local(sizes, tokens, gain1, in_w, group_w, pool_scale, out_w, gain2, up_w, down_w):
    n_rep, n_fs, n_tp = sizes
    rows, width = tokens.shape
    length, part = rows * n_tp, width // n_fs
    channels, hidden_units = in_w.shape[1], up_w.shape[1]
    bf16, f32 = jnp.bfloat16, jnp.float32
    weights = (in_w, out_w, up_w, down_w)
    vmem = pl.BlockSpec(memory_space=pltpu.VMEM)
    hbm = pl.BlockSpec(memory_space=pl.ANY)
    return pl.pallas_call(
        functools.partial(kernel, sizes),
        name="layer",
        out_shape=jax.ShapeDtypeStruct((rows, width), bf16),
        in_specs=[vmem, vmem, hbm, vmem, vmem, hbm, vmem, hbm, hbm],
        out_specs=vmem,
        scratch_shapes=[pltpu.VMEM((n_fs,) + w.shape, bf16) for w in weights]
        + [
            pltpu.VMEM((length, width), bf16),
            pltpu.VMEM((length, channels), f32),
            pltpu.VMEM((length, channels), bf16),
            pltpu.VMEM((n_fs, length, part), bf16),
            pltpu.VMEM((n_tp, n_fs, rows, part), bf16),
            pltpu.VMEM((n_fs, rows, part), f32),
            pltpu.VMEM((length, width), bf16),
            pltpu.VMEM((length, hidden_units), f32),
            pltpu.VMEM((length, hidden_units), bf16),
            pltpu.VMEM((n_fs, length, part), bf16),
            pltpu.VMEM((n_fs, n_tp, rows, part), bf16),
            pltpu.SemaphoreType.DMA((len(weights),)),
        ]
        + [
            pltpu.SemaphoreType.DMA((n_fs, 2 * n_rep + 2, chunks_of(*w.shape, n_rep)))
            for w in weights
        ]
        + [pltpu.SemaphoreType.DMA((3 + n_fs, n_tp))] * 2,
        compiler_params=pltpu.CompilerParams(
            collective_id=0, has_side_effects=True, vmem_limit_bytes=60 * 1024 * 1024
        ),
    )(
        tokens,
        gain1.reshape(1, -1),
        in_w,
        group_w,
        pool_scale.reshape(1, -1),
        out_w,
        gain2.reshape(1, -1),
        up_w,
        down_w,
    )


def solution(mesh):
    sizes = tuple(mesh.shape[axis] for axis in ("rep", "fs", "tp"))
    in_specs = (
        P(("rep", "fs", "tp"), None),
        P(),
        P("fs", "tp"),
        P("tp", None, None),
        P("tp"),
        P("tp", "fs"),
        P(),
        P("fs", "tp"),
        P("tp", "fs"),
    )
    return jax.shard_map(
        functools.partial(local, sizes),
        mesh=mesh,
        in_specs=in_specs,
        out_specs=P(("rep", "fs", "tp"), None),
        check_vma=False,
    )
```

```python
import functools

import jax
import jax.numpy as jnp
from jax import lax
from jax.experimental import pallas as pl
from jax.experimental.pallas import tpu as pltpu
from jax.sharding import PartitionSpec as P

MESH = pl.DeviceIdType.MESH
CHUNK_BYTES = 256 * 1024
LEVELS = 4

epsilon = 1e-06


def chunks_of(rows, columns, parts):
    count = max(1, rows * columns * 2 // parts // CHUNK_BYTES)
    while (rows // parts) % (count * 16):
        count -= 1
    return count


def column_chunks(rows, columns, parts):
    count = max(1, rows * columns * 2 // parts // CHUNK_BYTES)
    while count > 1 and columns % (count * 128):
        count -= 1
    return count


def chunk_counts_of(shapes, parts):
    counts = [chunks_of(*shape, parts) for shape in shapes[:3]]
    return counts + [column_chunks(*shapes[3], parts)]


def dot(a, b):
    return jnp.dot(a, b, preferred_element_type=jnp.float32)


def tile_of(columns, most):
    tile = min(columns, most)
    while columns % tile:
        tile //= 2
    return tile


def kernel(
    sizes,
    tokens,
    gain1,
    in_hbm,
    group_weight,
    pool_scale,
    out_hbm,
    gain2,
    up_hbm,
    down_hbm,
    result,
    in_buf,
    out_buf,
    up_buf,
    down_buf,
    normed,
    projected,
    pool_out,
    mix_send,
    mix_recv,
    stream2,
    normed2,
    upper,
    hidden,
    sum_send,
    sum_recv,
    local_sem,
    in_sems,
    out_sems,
    up_sems,
    down_sems,
    tp_send,
    tp_recv,
):
    n_rep, n_fs, n_tp = sizes
    r, f, t = lax.axis_index("rep"), lax.axis_index("fs"), lax.axis_index("tp")
    rows = tokens.shape[0]
    length = rows * n_tp
    width = tokens.shape[1]
    part = width // n_fs
    buffers = (in_buf, out_buf, up_buf, down_buf)
    sources = (in_hbm, out_hbm, up_hbm, down_hbm)
    sems = (
        in_sems,
        out_sems,
        up_sems,
        down_sems,
    )
    chunk_counts = chunk_counts_of([b.shape[1:] for b in buffers], n_rep)

    loads = []
    for index in range(4):
        load = pltpu.make_async_copy(sources[index], buffers[index].at[f], local_sem.at[index])
        load.start()
        loads.append(load)

    barrier = pltpu.get_barrier_semaphore()
    greeted = [{"fs": lax.rem(f + d, n_fs)} for d in (1, n_fs - 1)]
    greeted += [{"rep": lax.rem(r + d, n_rep)} for d in range(1, n_rep)]
    greeted += [{"tp": lax.rem(t + d, n_tp)} for d in range(1, n_tp)]
    for device in greeted:
        pl.semaphore_signal(barrier, inc=1, device_id=device, device_id_type=MESH)

    def order(p):
        nearest = jnp.minimum(f, n_fs - 1 - f)
        step = (p + 1) // 2
        near = f + step if p % 2 else f - step
        far = f + (p - nearest) * jnp.where(2 * f < n_fs, 1, -1)
        return jnp.where(p <= 2 * nearest, near, far)

    def piece(g, j, q, c):
        buf = buffers[g]
        if g == 3:
            half, block = buf.shape[1] // n_rep, buf.shape[2] // chunk_counts[g]
            start = pl.multiple_of(q * half, half)
            return buf.at[j, pl.ds(start, half), c * block : (c + 1) * block]
        size = buf.shape[1] // n_rep // chunk_counts[g]
        start = pl.multiple_of((q * chunk_counts[g] + c) * size, size)
        return buf.at[j, pl.ds(start, size), :]

    def remote(g, j, q, c, send_slot, device):
        block = piece(g, j, q, c)
        return pltpu.make_async_remote_copy(
            src_ref=block,
            dst_ref=block,
            send_sem=sems[g].at[j, send_slot, c],
            recv_sem=sems[g].at[j, q, c],
            device_id=device,
            device_id_type=MESH,
        )

    def along(g, j, c, way, act):
        if way == 0:

            @pl.when(f > 0)
            def _():
                act(remote(g, j, r, c, 2 * n_rep, {"fs": f - 1}))

        else:

            @pl.when(f < n_fs - 1)
            def _():
                act(remote(g, j, r, c, 2 * n_rep + 1, {"fs": f + 1}))

    def beside_end(j):
        return ((j == 0) & (f == 1)) | ((j == n_fs - 1) & (f == n_fs - 2))

    def whole_shard(g, c, act):
        for d in range(1, n_rep):
            other = lax.rem(r + d, n_rep)

            @pl.when(f == 0)
            def _():
                act(remote(g, f, other, c, n_rep + other, {"fs": f + 1}))

            @pl.when(f == n_fs - 1)
            def _():
                act(remote(g, f, other, c, n_rep + other, {"fs": f - 1}))

    def start(copy):
        copy.start()

    def drain(copy):
        copy.wait_send()

    def onward(g, p, c, act):
        j = order(p)

        @pl.when(j > f)
        def _():
            along(g, j, c, 0, act)

        @pl.when(j < f)
        def _():
            along(g, j, c, 1, act)

        @pl.when(jnp.logical_not(beside_end(j)))
        def _():
            for d in range(1, n_rep):
                other = lax.rem(r + d, n_rep)
                act(remote(g, j, r, c, n_rep + other, {"rep": other}))

    def send_own(g):
        for c in range(chunk_counts[g]):
            along(g, f, c, 0, start)
            along(g, f, c, 1, start)
        for c in range(chunk_counts[g]):
            whole_shard(g, c, start)

    def relay(g, p, work=()):
        work = list(work)
        for c in range(chunk_counts[g]):
            j = order(p)
            remote(g, j, r, c, 2 * n_rep, {"fs": f}).wait_recv()
            onward(g, p, c, start)
            if c < len(work):
                for action in work[c]:
                    action()

    def arrived(g, p):
        j = order(p)
        for d in range(1, n_rep):
            other = lax.rem(r + d, n_rep)
            for c in range(chunk_counts[g]):
                remote(g, j, other, c, n_rep + other, {"rep": other}).wait_recv()

    def block_of(index):
        return pl.ds(pl.multiple_of(index * rows, rows), rows)

    def tp_copies(kind, source, target):
        made = []
        for d in range(1, n_tp):
            other = lax.rem(t + d, n_tp)
            made.append(
                pltpu.make_async_remote_copy(
                    src_ref=source(other),
                    dst_ref=target(t),
                    send_sem=tp_send.at[kind, other],
                    recv_sem=tp_recv.at[kind, t],
                    device_id={"tp": other},
                    device_id_type=MESH,
                )
            )
        return made

    def tp_wait(kind, target):
        for d in range(1, n_tp):
            other = lax.rem(t + d, n_tp)
            pltpu.make_async_remote_copy(
                src_ref=target(other),
                dst_ref=target(other),
                send_sem=tp_send.at[kind, other],
                recv_sem=tp_recv.at[kind, other],
                device_id={"tp": other},
                device_id_type=MESH,
            ).wait_recv()

    stream = tokens[...].astype(jnp.float32)
    scale = lax.rsqrt(jnp.mean(stream * stream, axis=-1, keepdims=True) + epsilon)
    normed[block_of(t), :] = (stream * scale * gain1[...]).astype(jnp.bfloat16)

    pl.semaphore_wait(barrier, len(greeted))
    loads[0].wait()
    send_own(0)
    loads[1].wait()
    send_own(1)
    normed_at = lambda index: normed.at[block_of(index), :]
    sends = tp_copies(0, lambda other: normed_at(t), normed_at)
    for copy in sends:
        copy.start()
    for p in range(1, n_fs):
        relay(0, p)
        relay(1, p)
    loads[2].wait()
    send_own(2)

    tp_wait(0, normed_at)
    for p in range(1, n_fs):
        arrived(0, p)
    total = dot(normed[:, :part], in_buf[0])
    for index in range(1, n_fs):
        total += dot(normed[:, index * part : (index + 1) * part], in_buf[index])
    projected[...] = total.astype(jnp.bfloat16).astype(jnp.float32)
    groups, channels = group_weight.shape[0], group_weight.shape[1]
    position = lax.broadcasted_iota(jnp.int32, (length, channels), 0)
    for group in range(groups):
        lanes = slice(group * channels, (group + 1) * channels)
        values = projected[:, lanes]
        level_of = jnp.full((length, channels), lax.rem(t * groups + group, LEVELS), jnp.int32)
        running = values
        mean = jnp.zeros_like(values)
        for level in range(LEVELS):
            offset = 2**level
            running = running + jnp.where(position >= offset, pltpu.roll(running, offset, 0), 0.0)
            count = jnp.minimum(position + 1, 2 * offset).astype(jnp.float32)
            mean = jnp.where(level_of == level, running / count, mean)
        pooled = (mean - values).astype(jnp.bfloat16)
        mapped = dot(pooled, group_weight[group])
        pool_out[:, lanes] = (mapped * pool_scale[:, lanes]).astype(jnp.bfloat16)

    for p in range(1, n_fs):
        arrived(1, p)
    for index in range(n_fs):
        mix_send[index] = dot(pool_out[...], out_buf[index]).astype(jnp.bfloat16)
    more = tp_copies(
        1, lambda other: mix_send.at[:, block_of(other), :], lambda index: mix_recv.at[index]
    )
    for copy in more:
        copy.start()
    sends += more
    for p in range(1, n_fs):
        relay(2, p)
    loads[3].wait()
    send_own(3)

    tp_wait(1, lambda index: mix_recv.at[index])
    square = jnp.zeros((rows, 1), jnp.float32)
    for index in range(n_fs):
        mixed = tokens[:, index * part : (index + 1) * part].astype(jnp.float32)
        mixed += mix_send[index, block_of(t), :].astype(jnp.float32)
        for d in range(1, n_tp):
            mixed += mix_recv[lax.rem(t + d, n_tp), index].astype(jnp.float32)
        stream2[index] = mixed
        square += jnp.sum(mixed * mixed, axis=-1, keepdims=True)
    scale = lax.rsqrt(square / width + epsilon)
    for index in range(n_fs):
        columns = slice(index * part, (index + 1) * part)
        normed2[block_of(t), columns] = (stream2[index] * scale * gain2[:, columns]).astype(
            jnp.bfloat16
        )
    normed2_at = lambda index: normed2.at[block_of(index), :]
    more = tp_copies(2, lambda other: normed2_at(t), normed2_at)
    for copy in more:
        copy.start()
    sends += more
    relay(3, 1)

    tp_wait(2, normed2_at)
    up_columns = up_buf.shape[2]
    up_tile = tile_of(up_columns, 512)

    def up_product(p):
        j = order(p)
        left = normed2.at[:, pl.ds(pl.multiple_of(j * part, part), part)]

        @pl.loop(0, up_columns // up_tile)
        def _(i):
            columns = pl.ds(pl.multiple_of(i * up_tile, up_tile), up_tile)
            product = dot(left[...], up_buf[j, :, columns])
            if p == 0:
                upper[:, columns] = product
            elif p < n_fs - 1:
                upper[:, columns] += product
            else:
                value = jnp.maximum(upper[:, columns] + product, 0.0)
                hidden[:, columns] = (value * value).astype(jnp.bfloat16)

    def up_work(p):
        if p:
            arrived(2, p)
        up_product(p)

    down_tile = tile_of(part, 256)

    def sum_kind(p):
        return 3 + p

    def down_product(p):
        j = order(p)

        @pl.loop(0, part // down_tile)
        def _(i):
            columns = pl.ds(pl.multiple_of(i * down_tile, down_tile), down_tile)
            sum_send[p, :, columns] = dot(hidden[...], down_buf[j, :, columns]).astype(jnp.bfloat16)

        copies = tp_copies(
            sum_kind(p),
            lambda other: sum_send.at[p, block_of(other), :],
            lambda index: sum_recv.at[p, index],
        )
        for copy in copies:
            copy.start()
        return copies

    def finish(p):
        j = order(p)
        tp_wait(sum_kind(p), lambda index: sum_recv.at[p, index])
        channel = sum_send[p, block_of(t), :].astype(jnp.float32)
        for d in range(1, n_tp):
            channel += sum_recv[p, lax.rem(t + d, n_tp)].astype(jnp.float32)
        columns = pl.ds(pl.multiple_of(j * part, part), part)
        result[:, columns] = (stream2[j] + channel).astype(jnp.bfloat16)

    def down_work(p):
        if p:
            arrived(3, p)
        sends.extend(down_product(p))
        if p:
            finish(p - 1)

    count = chunk_counts[3]
    block = part // count
    last = n_fs - 1

    def last_work(c):
        j = order(last)
        for d in range(1, n_rep):
            other = lax.rem(r + d, n_rep)
            remote(3, j, other, c, n_rep + other, {"rep": other}).wait_recv()
        columns = slice(c * block, (c + 1) * block)
        product = dot(hidden[...], down_buf[j, :, columns])
        sum_send[last, :, columns] = product.astype(jnp.bfloat16)
        copies = tp_copies(
            sum_kind(last) + c,
            lambda other: sum_send.at[last, block_of(other), columns],
            lambda index: sum_recv.at[last, index, :, columns],
        )
        for copy in copies:
            copy.start()
        sends.extend(copies)

    def last_finish(c):
        j = order(last)
        columns = slice(c * block, (c + 1) * block)
        tp_wait(sum_kind(last) + c, lambda index: sum_recv.at[last, index, :, columns])
        channel = sum_send[last, block_of(t), columns].astype(jnp.float32)
        for d in range(1, n_tp):
            channel += sum_recv[last, lax.rem(t + d, n_tp), :, columns].astype(jnp.float32)
        place = pl.ds(pl.multiple_of(j * part + c * block, block), block)
        result[:, place] = (stream2[j, :, columns] + channel).astype(jnp.bfloat16)

    ups = [functools.partial(up_work, p) for p in range(n_fs)]
    downs = [functools.partial(down_work, p) for p in range(last)]
    lasts = [functools.partial(last_work, c) for c in range(count)]
    for p in range(2, n_fs):
        if ups:
            step = -(-len(ups) // count)
            relay(3, p, [ups[i : i + step] for i in range(0, len(ups), step)])
            ups = []
        elif p < last:
            relay(3, p, [downs[:1]])
            downs = downs[1:]
        else:
            plan = [[] for _ in range(count)]
            half = (len(downs) + 1) // 2
            plan[0] = downs[:half]
            plan[min(1, count - 1)] = plan[min(1, count - 1)] + downs[half:]
            if count == 1:
                plan[0] = downs
            for c in range(2, count):
                plan[c] = [lasts.pop(0)]
            relay(3, p, plan)
            downs = []
    for work in ups + downs + lasts:
        work()
    finish(last - 1)
    for g in range(4):
        for c in range(chunk_counts[g]):
            along(g, f, c, 0, drain)
            along(g, f, c, 1, drain)
            whole_shard(g, c, drain)
            for p in range(1, n_fs):
                onward(g, p, c, drain)
    for c in range(count):
        last_finish(c)
    for copy in sends:
        copy.wait_send()


def local(sizes, tokens, gain1, in_w, group_w, pool_scale, out_w, gain2, up_w, down_w):
    n_rep, n_fs, n_tp = sizes
    rows, width = tokens.shape
    length, part = rows * n_tp, width // n_fs
    channels, hidden_units = in_w.shape[1], up_w.shape[1]
    bf16, f32 = jnp.bfloat16, jnp.float32
    weights = (in_w, out_w, up_w, down_w)
    counts = chunk_counts_of([w.shape for w in weights], n_rep)
    vmem = pl.BlockSpec(memory_space=pltpu.VMEM)
    hbm = pl.BlockSpec(memory_space=pl.ANY)
    return pl.pallas_call(
        functools.partial(kernel, sizes),
        name="layer",
        out_shape=jax.ShapeDtypeStruct((rows, width), bf16),
        in_specs=[vmem, vmem, hbm, vmem, vmem, hbm, vmem, hbm, hbm],
        out_specs=vmem,
        scratch_shapes=[pltpu.VMEM((n_fs,) + w.shape, bf16) for w in weights]
        + [
            pltpu.VMEM((length, width), bf16),
            pltpu.VMEM((length, channels), f32),
            pltpu.VMEM((length, channels), bf16),
            pltpu.VMEM((n_fs, length, part), bf16),
            pltpu.VMEM((n_tp, n_fs, rows, part), bf16),
            pltpu.VMEM((n_fs, rows, part), f32),
            pltpu.VMEM((length, width), bf16),
            pltpu.VMEM((length, hidden_units), f32),
            pltpu.VMEM((length, hidden_units), bf16),
            pltpu.VMEM((n_fs, length, part), bf16),
            pltpu.VMEM((n_fs, n_tp, rows, part), bf16),
            pltpu.SemaphoreType.DMA((len(weights),)),
        ]
        + [
            pltpu.SemaphoreType.DMA((n_fs, 2 * n_rep + 2, count)) for count in counts
        ]
        + [pltpu.SemaphoreType.DMA((2 + n_fs + counts[3], n_tp))] * 2,
        compiler_params=pltpu.CompilerParams(
            collective_id=0, has_side_effects=True, vmem_limit_bytes=60 * 1024 * 1024
        ),
    )(
        tokens,
        gain1.reshape(1, -1),
        in_w,
        group_w,
        pool_scale.reshape(1, -1),
        out_w,
        gain2.reshape(1, -1),
        up_w,
        down_w,
    )


def solution(mesh):
    sizes = tuple(mesh.shape[axis] for axis in ("rep", "fs", "tp"))
    in_specs = (
        P(("rep", "fs", "tp"), None),
        P(),
        P("fs", "tp"),
        P("tp", None, None),
        P("tp"),
        P("tp", "fs"),
        P(),
        P("fs", "tp"),
        P("tp", "fs"),
    )
    return jax.shard_map(
        functools.partial(local, sizes),
        mesh=mesh,
        in_specs=in_specs,
        out_specs=P(("rep", "fs", "tp"), None),
        check_vma=False,
    )
```
